32 devices in a mesh: ep: 8 (over z, core), tp: 4 (over y, x).
Axes of the slice: x: 2, y: 2, z: 4, core: 2. Of those that a mesh axis runs over, the one named last changes fastest.
Arguments:
- resid: bfloat16 [64, 2048], P('ep', 'tp'), may hold values from -6 to 6
- attn_gain: float32 [2048], replicated, may hold values from 0.1 to 1.9
- w_query: bfloat16 [2048, 1024], P(None, 'tp'), may hold values from -0.125 to 0.125
- w_key: bfloat16 [2048, 1024], P(None, 'tp'), may hold values from -0.125 to 0.125
- w_value: bfloat16 [2048, 1024], P(None, 'tp'), may hold values from -0.125 to 0.125
- key_cache: bfloat16 [64, 16, 64, 1024], P('ep', 'tp'), may hold values from -6 to 6
- value_cache: bfloat16 [64, 16, 64, 1024], P('ep', 'tp'), may hold values from -19 to 19
- key_bias: float32 [64, 16, 1024], P('ep', 'tp'), may hold values from -10.2 to 0
- lengths: int32 [64], P('ep'), may hold values from 1 to 1024
- mix_gain: float32 [1024], P('tp'), may hold values from 0.1 to 1.9
- w_out: bfloat16 [1024, 2048], P('tp'), may hold values from -0.1875 to 0.1875
- ffn_gain: float32 [2048], replicated, may hold values from 0.1 to 1.9
- route_experts: int32 [64, 4], P('ep'), may hold values from 0 to 7, all different within a row; in each aligned block of 8 rows (0 to 7, 8 to 15, ...) at most 8 rows name the same one
- route_weights: float32 [64, 4], P('ep'), may hold values from 0.05 to 1
- w_gate: bfloat16 [8, 2048, 2048], P('ep', None, 'tp'), may hold values from -0.3125 to 0.3125
- w_up: bfloat16 [8, 2048, 2048], P('ep', None, 'tp'), may hold values from -0.3125 to 0.3125
- w_down: bfloat16 [8, 2048, 2048], P('ep', 'tp'), may hold values from -0.0546875 to 0.0546875
Outputs:
- mixed: bfloat16 [64, 2048], P('ep', 'tp')
- new_keys: bfloat16 [64, 1024], P('ep', 'tp')
- new_values: bfloat16 [64, 1024], P('ep', 'tp')
The draws below stay inside these ranges and needn't reach their ends.
Inputs may be any that keep to these rules, and one draw needn't show every extreme that they name: `route_experts`: each row names 4 different experts. Within the rows of one device (aligned blocks of 8 rows) no expert is named more than 8 times, a bound that some block reaches.
All inputs are finite; a program needn't handle non-finite values.
Results may differ from the reference program's by a relative error of at most 0.018.
Values may be sent and summed in bfloat16 or wider, within the bound.
A program may use at most 64 MiB of HBM per device.

```python
import math
import jax
import jax.numpy as jnp
import numpy as np
from jax import lax

D = 2048
QUERY_GROUPS = 16
HEAD_DIM = 64
FF = 2048
TOP_K = 4
SEQS = 8
STORED_SLOTS = 1024
EXPERTS = 8
BATCH_STREAMS = 64
CAP = 8
SLICES = 4
N_EP = 8


def draw_value_cache(key, part):
    noise = jax.random.normal(jax.random.fold_in(key, 11), (BATCH_STREAMS, QUERY_GROUPS, HEAD_DIM, STORED_SLOTS), jnp.float32)
    center = 0.7 * jax.random.normal(jax.random.fold_in(key, 12), (BATCH_STREAMS, QUERY_GROUPS, HEAD_DIM, 1), jnp.float32)
    levels = 10.0 ** (0.5 * jnp.arange(QUERY_GROUPS, dtype=jnp.float32) / max(QUERY_GROUPS - 1, 1))
    values = jnp.clip(center + noise, -6.0, 6.0) * levels[None, :, None, None]
    return values.astype(jnp.bfloat16)


def draw_key_bias(key, part):
    slow_share = 0.5
    slow = jax.random.uniform(jax.random.fold_in(key, 21), (BATCH_STREAMS, QUERY_GROUPS), jnp.float32) < slow_share
    slow_base = jax.random.uniform(jax.random.fold_in(key, 22), (BATCH_STREAMS, QUERY_GROUPS), jnp.float32, -8.5, -7.0)
    fast_base = jax.random.uniform(jax.random.fold_in(key, 23), (BATCH_STREAMS, QUERY_GROUPS), jnp.float32, -3.5, -2.5)
    tilt = jax.random.uniform(jax.random.fold_in(key, 24), (BATCH_STREAMS, 1), jnp.float32, -0.7, 0.7)
    approximate_guess = jax.random.uniform(jax.random.fold_in(key, 25), (BATCH_STREAMS, QUERY_GROUPS, STORED_SLOTS), jnp.float32, -1.0, 1.0)
    spike_magnitude = jax.random.uniform(jax.random.fold_in(key, 26), (BATCH_STREAMS, QUERY_GROUPS, STORED_SLOTS), jnp.float32) < 3.0 / STORED_SLOTS
    raised_entries = jax.random.uniform(jax.random.fold_in(key, 27), (BATCH_STREAMS, QUERY_GROUPS, STORED_SLOTS), jnp.float32, -1.5, 0.0)
    floor_offset = jnp.where(slow, slow_base, fast_base) + tilt
    return jnp.where(spike_magnitude, raised_entries, floor_offset[:, :, None] + approximate_guess).astype(jnp.float32)


def place_ends(array, rng, least, top_value):
    extent = array.shape
    place = [jax.random.randint(jax.random.fold_in(rng, axis), (), 0, extent[axis]) for axis in range(len(extent))]
    array = array.at[tuple(place)].set(least)
    longest = extent.index(max(extent))
    place[longest] = (place[longest] + 1) % extent[longest]
    return array.at[tuple(place)].set(top_value)


def level_of(key, shape, cuts, least, top_value):
    def one(dim, shards_of):
        steps = jax.random.uniform(jax.random.fold_in(jax.random.fold_in(key, 6), dim), (shards_of,), jnp.float32, least / len(cuts), top_value / len(cuts))
        return jnp.repeat(jnp.exp(steps), shape[dim] // shards_of).reshape((-1,) + (1,) * (len(shape) - dim - 1))

    factor_of = one(*cuts[0])
    for cut in cuts[1:]:
        factor_of = factor_of * one(*cut)
    return factor_of


def shared_out(stream_key, own, number, rows, amount, top, most, lean):
    sequence = jax.random.permutation(stream_key, amount)
    crowded, common = load_shares(amount, rows * top, most, lean, True), load_shares(amount, rows * top, most, lean, False)
    places = jnp.arange(amount)

    def named(sizes, offset_by):
        used = int((sizes > 0).sum())
        fixed = max(1, used // 4)
        shifted = fixed + (places - fixed + offset_by * (used - fixed)) % max(1, amount - fixed)
        return jnp.zeros((amount,), jnp.int32).at[sequence[jnp.where(places < fixed, places, shifted)]].set(jnp.asarray(sizes, jnp.int32))

    sizes = jnp.where(number % 4 == 0, named(crowded, number // 4), named(common, number - number // 4 - 1))
    mixed = jax.random.permutation(jax.random.fold_in(own, 3), amount)
    donor, taker = mixed[0:amount // 2 * 2:2], mixed[1:amount // 2 * 2:2]
    room = jnp.minimum(sizes[donor] - 1, most - sizes[taker]) // 2
    room = jnp.where((donor == sequence[0]) | (taker == sequence[0]) | (sizes[taker] == 0), 0, jnp.maximum(room, 0))
    shifted = jax.random.randint(jax.random.fold_in(own, 4), (amount // 2,), 0, 1 << 20) % (room + 1)
    sizes = sizes.at[donor].add(-shifted).at[taker].add(shifted)
    labels = jnp.searchsorted(jnp.cumsum(sizes), jnp.arange(rows * top), side="right").astype(jnp.int32)
    listing = labels.reshape(top, rows).T
    listing = listing[jax.random.permutation(jax.random.fold_in(own, 1), rows)]
    offset_by = jax.random.randint(jax.random.fold_in(own, 2), (rows, 1), 0, top)
    return jnp.take_along_axis(listing, (jnp.arange(top)[None, :] + offset_by) % top, axis=1)


def load_shares(number_of, total, bound, slope, full):
    portions = [(1 << 20) // math.isqrt(grade ** slope) + 1 for grade in range(1, number_of + 1)]
    largest = bound if full else min(bound, max(-(-total // number_of), total * portions[0] // sum(portions)))
    least = 1 if total - largest >= number_of - 1 else 0
    given, spare = [largest] + [least] * (number_of - 1), total - largest - least * (number_of - 1)
    while spare > 0:
        movable = [i for i in range(1, number_of) if given[i] < largest] or [i for i in range(1, number_of) if given[i] < bound]
        mass, budget = sum([portions[i] for i in movable]), spare
        for i in movable:
            more = min(bound - given[i], max(1, budget * portions[i] // mass), spare)
            given[i] = given[i] + more
            spare = spare - more
    return np.array(given)


def scatter_about(rng, shape, scale, most, shards=(), kind=jnp.bfloat16):
    level = level_of(rng, shape, shards, -0.22, 0.18) if shards else 1.0
    entries = jax.random.normal(rng, shape, jnp.float32) * scale * level
    return jnp.minimum(jnp.maximum(entries, -most), most).astype(kind)


def setup_inputs(seed: int = 0) -> dict:
    seeds = jax.random.split(jax.random.key(seed), 18)
    resid = scatter_about(seeds[0], (BATCH_STREAMS, D), 1.0, 6.0, ((0, 8), (1, 4)))
    attn_gain = jnp.clip(1.0 + 0.18 * jax.random.normal(seeds[1], (D,), jnp.float32), 0.1, 1.9)
    w_query = scatter_about(seeds[2], (D, QUERY_GROUPS * HEAD_DIM), D ** -0.5, 0.125, ((1, 4),))
    w_key = scatter_about(seeds[3], (D, QUERY_GROUPS * HEAD_DIM), D ** -0.5, 0.125, ((1, 4),))
    w_value = scatter_about(seeds[4], (D, QUERY_GROUPS * HEAD_DIM), D ** -0.5, 0.125, ((1, 4),))
    key_cache = scatter_about(seeds[5], (BATCH_STREAMS, QUERY_GROUPS, HEAD_DIM, STORED_SLOTS), 1.0, 6.0, ((0, 8), (1, 4)))
    value_cache = draw_value_cache(jax.random.fold_in(seeds[17], 71), 0)
    key_bias = draw_key_bias(jax.random.fold_in(seeds[17], 71), 0)
    lengths = place_ends(jax.random.randint(seeds[8], (BATCH_STREAMS,), 1, STORED_SLOTS + 1), jax.random.fold_in(seeds[8], 1), 1, STORED_SLOTS).astype(jnp.int32)
    mix_gain = jnp.clip(1.0 + 0.18 * jax.random.normal(seeds[9], (QUERY_GROUPS * HEAD_DIM,), jnp.float32), 0.1, 1.9)
    w_out = scatter_about(seeds[10], (QUERY_GROUPS * HEAD_DIM, D), (QUERY_GROUPS * HEAD_DIM) ** -0.5, 0.1875, ((0, 4),))
    ffn_gain = jnp.clip(1.0 + 0.18 * jax.random.normal(seeds[11], (D,), jnp.float32), 0.1, 1.9)
    route_experts_keys = jax.random.split(jax.random.fold_in(seeds[12], 1), BATCH_STREAMS // SEQS)
    route_experts_turns = jax.random.permutation(jax.random.fold_in(seeds[12], 3), BATCH_STREAMS // SEQS)
    route_experts = jax.vmap(lambda own, number: shared_out(jax.random.fold_in(seeds[12], 2), own, number, SEQS, EXPERTS, TOP_K, CAP, 2))(route_experts_keys, route_experts_turns).reshape((BATCH_STREAMS, TOP_K))
    route_weights = jnp.clip(jnp.exp(math.log(1.0) - 2.9957323 * jax.random.uniform(seeds[13], (BATCH_STREAMS, TOP_K), jnp.float32) ** level_of(seeds[13], (BATCH_STREAMS, TOP_K), ((0, 8),), -0.2, 0.2)), 0.05, 1.0)
    w_gate = scatter_about(seeds[14], (EXPERTS, D, FF), (2.5 / D ** 0.5), 0.3125, ((0, 8), (2, 4)))
    w_up = scatter_about(seeds[15], (EXPERTS, D, FF), (2.5 / D ** 0.5), 0.3125, ((0, 8), (2, 4)))
    w_down = scatter_about(seeds[16], (EXPERTS, FF, D), (0.4 / FF ** 0.5), 0.0546875, ((0, 8), (1, 4)))
    return {"resid": resid, "attn_gain": attn_gain, "w_query": w_query, "w_key": w_key, "w_value": w_value, "key_cache": key_cache, "value_cache": value_cache, "key_bias": key_bias, "lengths": lengths, "mix_gain": mix_gain, "w_out": w_out, "ffn_gain": ffn_gain, "route_experts": route_experts, "route_weights": route_weights, "w_gate": w_gate, "w_up": w_up, "w_down": w_down}


eps = 1e-06
limit = 7.0
alpha = 1.702

def rms_rows(values, gain):
    return values * lax.rsqrt(lax.optimization_barrier(jnp.mean(values * values, axis=-1, keepdims=True)) + eps) * gain

def stick_one(query, keys, values, bias, length):
    scores = jnp.einsum('hd,hds->hs', query.astype(jnp.float32), keys.astype(jnp.float32)) * HEAD_DIM ** (-0.5) + bias
    live = jnp.arange(STORED_SLOTS, dtype=jnp.int32)[None, :] < length
    log_keep = jnp.where(live, jax.nn.log_sigmoid(-scores), 0.0)
    after = lax.cumsum(log_keep, axis=1, reverse=True) - log_keep
    weights = jnp.where(live, jnp.exp(jax.nn.log_sigmoid(scores) + after), 0.0).astype(jnp.bfloat16)
    return jnp.einsum('hs,hds->hd', weights.astype(jnp.float32), values.astype(jnp.float32))

def reference(resid, attn_gain, w_query, w_key, w_value, key_cache, value_cache, key_bias, lengths, mix_gain, w_out, ffn_gain, route_experts, route_weights, w_gate, w_up, w_down):
    whole = resid.astype(jnp.float32)
    normed_in = rms_rows(whole, attn_gain).astype(jnp.bfloat16)
    query = jnp.dot(normed_in, w_query, preferred_element_type=jnp.float32).astype(jnp.bfloat16)
    new_keys = jnp.dot(normed_in, w_key, preferred_element_type=jnp.float32).astype(jnp.bfloat16)
    new_values = jnp.dot(normed_in, w_value, preferred_element_type=jnp.float32).astype(jnp.bfloat16)
    head_query = query.reshape(BATCH_STREAMS, QUERY_GROUPS, HEAD_DIM)

    def attend(item):
        return stick_one(item[0], item[1], item[2], item[3], item[4])
    attended = lax.map(attend, (head_query, key_cache, value_cache, key_bias, lengths)).reshape(BATCH_STREAMS, QUERY_GROUPS * HEAD_DIM)
    normed_heads = rms_rows(attended, mix_gain).astype(jnp.bfloat16)
    block = QUERY_GROUPS * HEAD_DIM // SLICES
    partial_heads = jnp.einsum('njr,jrd->njd', normed_heads.reshape(BATCH_STREAMS, SLICES, block).astype(jnp.float32), w_out.reshape(SLICES, block, D).astype(jnp.float32))
    partial_heads = lax.optimization_barrier(partial_heads.astype(jnp.bfloat16)).astype(jnp.float32)
    middle = whole + lax.optimization_barrier(jnp.sum(partial_heads, axis=1))
    normed_mid = rms_rows(middle, ffn_gain).astype(jnp.bfloat16)
    share = route_weights / lax.optimization_barrier(jnp.sum(route_weights, axis=1, keepdims=True))
    chosen = route_experts.reshape(N_EP, SEQS * TOP_K)
    position = jnp.arange(SEQS * TOP_K, dtype=jnp.int32)
    earlier = (chosen[:, :, None] == chosen[:, None, :]) & (position[:, None] > position[None, :])[None]
    rank = lax.optimization_barrier(jnp.sum(earlier.astype(jnp.int32), axis=2))
    slot = (jnp.arange(N_EP, dtype=jnp.int32)[:, None] * CAP + rank).reshape(-1)
    expert_flat = route_experts.reshape(-1)
    token_flat = jnp.repeat(jnp.arange(BATCH_STREAMS, dtype=jnp.int32), TOP_K)
    table = jnp.zeros((EXPERTS, N_EP * CAP), jnp.int32).at[expert_flat, slot].set(token_flat)
    hidden_block = FF // SLICES

    def one_expert(item):
        gate_weight, up_weight, down_weight, row_index = item
        inputs = normed_mid[row_index]
        gate = jnp.minimum(jnp.dot(inputs, gate_weight, preferred_element_type=jnp.float32), limit)
        upper = jnp.clip(jnp.dot(inputs, up_weight, preferred_element_type=jnp.float32), -limit, limit)
        active = ((upper + 1.0) * gate * jax.nn.sigmoid(alpha * gate)).astype(jnp.bfloat16)
        pieces = jnp.einsum('sjf,jfd->sjd', active.reshape(-1, SLICES, hidden_block).astype(jnp.float32), down_weight.reshape(SLICES, hidden_block, D).astype(jnp.float32))
        pieces = lax.optimization_barrier(pieces.astype(jnp.bfloat16)).astype(jnp.float32)
        return lax.optimization_barrier(jnp.sum(pieces, axis=1)).astype(jnp.bfloat16)
    outputs = lax.map(one_expert, (w_gate, w_up, w_down, table))
    picked = outputs[expert_flat, slot].astype(jnp.float32).reshape(BATCH_STREAMS, TOP_K, D)
    mixture = lax.optimization_barrier(jnp.sum(share[:, :, None] * picked, axis=1))
    mixed = (middle + mixture).astype(jnp.bfloat16)
    return (mixed, new_keys, new_values)
```

```python
import functools

import jax
import jax.numpy as jnp
from jax import lax
from jax.experimental import pallas as pl
from jax.experimental.pallas import tpu as pltpu
from jax.sharding import PartitionSpec as P

eps = 1e-06
limit = 7.0
alpha = 1.702
LIMIT_A = 48
LIMIT_B = 48
MESH = pl.DeviceIdType.MESH
F32 = jnp.float32
BF16 = jnp.bfloat16


def mm(a, b):
    return jnp.dot(a, b, preferred_element_type=F32)


def mm_nt(a, b):
    return lax.dot_general(a, b, (((1,), (1,)), ((), ())), preferred_element_type=F32)


def mm(a, b):
    return jnp.dot(a, b, preferred_element_type=F32)


def mm_nt(a, b):
    return lax.dot_general(a, b, (((1,), (1,)), ((), ())), preferred_element_type=F32)


_cur=[None]
def mark(name):
    if _cur[0] is not None:
        _cur[0].__exit__(None,None,None)
        _cur[0]=None
    if name:
        _cur[0]=jax.named_scope(name); _cur[0].__enter__()


def near_first(z, chips, k):
    if k == 0:
        return z
    room = jnp.minimum(z, chips - 1 - z)
    step = (k + 1) // 2
    both = z + step if k % 2 else z - step
    single = jnp.where(z < chips - 1 - z, z + (k - room), z - (k - room))
    return jnp.where(k <= 2 * room, both, single)


def peer_of(t, d, tp):
    if tp & (tp - 1):
        return lax.rem(t + d, tp)
    out = t
    bit = 1
    while bit < tp:
        if d & bit:
            out = out + bit - 2 * bit * lax.rem(out // bit, 2)
        bit *= 2
    return out


def start_loads(sem, groups):
    loads = []
    for i, group in enumerate(groups):
        copies = [pltpu.make_async_copy(src, dst, sem.at[i]) for src, dst in group]
        for copy in copies:
            copy.start()
        loads.append(copies)

    def loaded(i):
        for copy in loads[i]:
            copy.wait()

    return loaded


def gather(
    tp,
    h_resid, h_lengths, h_attn_gain, h_wq, h_key, h_value, h_bias,
    gathered, attn_gain, wq, key, value, bias_rows, limits,
    resid, lengths, bias, load_sem, send_sem, recv_sem,
):
    t = lax.axis_index("tp")
    seqs, heads, _ = bias.shape
    barrier = pltpu.get_barrier_semaphore()
    for d in range(1, tp):
        pl.semaphore_signal(barrier, inc=1, device_id={"tp": peer_of(t, d, tp)}, device_id_type=MESH)
    loaded = start_loads(load_sem, (
        ((h_resid, resid),),
        ((h_bias, bias), (h_lengths, lengths)),
        ((h_attn_gain, attn_gain), (h_wq, wq), (h_key, key), (h_value, value)),
    ))
    loaded(0)
    pl.semaphore_wait(barrier, tp - 1)

    def copy_to(d):
        return pltpu.make_async_remote_copy(
            src_ref=resid, dst_ref=gathered.at[t], send_sem=send_sem, recv_sem=recv_sem.at[d],
            device_id={"tp": peer_of(t, d, tp)}, device_id_type=MESH,
        )

    copies = [copy_to(d) for d in reversed(range(1, tp))]
    for copy in copies:
        copy.start()
    gathered[t] = resid[...]
    loaded(1)
    for n in range(seqs):
        bias_rows[pl.ds(n * heads, heads), :] = bias[n]
    row = lax.broadcasted_iota(jnp.int32, limits.shape, 0)
    limit_rows = jnp.zeros(limits.shape, jnp.int32)
    for n in range(seqs):
        limit_rows = jnp.where(row // heads == n, lengths[n], limit_rows)
    limits[...] = limit_rows
    loaded(2)
    for copy in copies:
        copy.wait_recv()
    for copy in copies:
        copy.wait_send()


def layer(
    tp, ep, heads, width,
    gathered, attn_gain, wq, key, value, bias_rows, limits,
    h_mix_gain, h_ffn_gain, h_experts, h_weights, h_wo, h_gate, h_up, h_wk, h_wv, h_down,
    mixed, new_keys, new_values,
    mix_gain, ffn_gain, route_experts, route_weights, wo, gate_w, up_w, wk, wv, down_w,
    branch, mid, tokens, pieces, arrived, outs, back,
    load_sem, send_sem, br_recv, tok_recv, fwd_recv, down_recv, ret_recv,
):
    t = lax.axis_index("tp")
    e = lax.axis_index("ep")
    chips = ep // 2
    z, core = e // 2, lax.rem(e, 2)
    _, seqs, shard = gathered.shape
    model = tp * shard
    span = heads * width
    rows = seqs * heads
    cache = key.shape[1]

    def tp_peer(d):
        return {"tp": peer_of(t, d, tp)}

    def ep_peer(d):
        return {"ep": lax.rem(e + d, ep)}

    sent = []

    def remote(src, dst, recv, device):
        return pltpu.make_async_remote_copy(
            src_ref=src, dst_ref=dst, send_sem=send_sem, recv_sem=recv, device_id=device, device_id_type=MESH
        )

    def send(src, dst, recv, device):
        copy = remote(src, dst, recv, device)
        copy.start()
        sent.append(copy)
        return copy

    barrier = pltpu.get_barrier_semaphore()
    for d in range(1, ep):
        pl.semaphore_signal(barrier, inc=1, device_id=ep_peer(d), device_id_type=MESH)
    for d in range(1, tp):
        pl.semaphore_signal(barrier, inc=1, device_id=tp_peer(d), device_id_type=MESH)
    loaded = start_loads(load_sem, (
        ((h_mix_gain, mix_gain), (h_wo, wo)),
        ((h_ffn_gain, ffn_gain), (h_experts, route_experts), (h_weights, route_weights), (h_wk, wk), (h_wv, wv)),
        ((h_gate.at[0], gate_w), (h_up.at[0], up_w), (h_down.at[0], down_w)),
    ))

    live = lax.broadcasted_iota(jnp.int32, (rows, cache), 1) < limits[:, 0:1]
    own_row = lax.broadcasted_iota(jnp.int32, (rows, span), 0)
    own_head = lax.broadcasted_iota(jnp.int32, (rows, span), 1) // width
    repeat = (
        lax.broadcasted_iota(jnp.int32, (rows, seqs), 0) // heads
        == lax.broadcasted_iota(jnp.int32, (rows, seqs), 1)
    ).astype(F32).astype(BF16)
    block = min(256, cache)
    blocks = cache // block
    lower = (
        lax.broadcasted_iota(jnp.int32, (block, block), 0)
        >= lax.broadcasted_iota(jnp.int32, (block, block), 1)
    ).astype(F32).astype(BF16)

    whole = jnp.concatenate([gathered[j].astype(F32) for j in range(tp)], axis=1)
    normed_in = (
        whole * lax.rsqrt(jnp.mean(whole * whole, axis=1, keepdims=True) + eps) * attn_gain[...]
    ).astype(BF16)
    query = mm(normed_in, wq[...]).astype(BF16)

    spread = mm(repeat, query)
    masked = jnp.concatenate(
        [jnp.where(own_row == n * heads + own_head, spread, 0.0).astype(BF16) for n in range(seqs)], axis=1
    )
    scores = mm(masked, key[...]) * width ** (-0.5) + bias_rows[...]
    soft = jnp.maximum(scores, 0.0) + jnp.log1p(jnp.exp(-jnp.abs(scores)))
    soft = jnp.where(live, soft, 0.0)
    stacked = jnp.concatenate([soft[:, b * block:(b + 1) * block] for b in range(blocks)], axis=0)
    high = stacked.astype(BF16)
    rest = stacked - high.astype(F32)
    middle_part = rest.astype(BF16)
    low = (rest - middle_part.astype(F32)).astype(BF16)
    within = mm(high, lower) + mm(middle_part, lower) + mm(low, lower)
    later = jnp.zeros((rows, 1), F32)
    suffix = [None] * blocks
    for b in reversed(range(blocks)):
        part = within[b * rows:(b + 1) * rows]
        suffix[b] = part + later
        later = later + part[:, 0:1]
    suffix = jnp.concatenate(suffix, axis=1)
    stick = jnp.where(live, jnp.exp(scores - suffix), 0.0).astype(BF16)

    seq_row = lax.broadcasted_iota(jnp.int32, (seqs, span), 0)
    attended = jnp.zeros((seqs, span), F32)
    whole_product = mm_nt(stick, value[...])
    for n in range(seqs):
        product = whole_product[:, n * span:(n + 1) * span]
        product = jnp.where(own_row == n * heads + own_head, product, 0.0)
        attended = jnp.where(seq_row == n, jnp.sum(product, axis=0, keepdims=True), attended)

    square = jnp.sum(attended * attended, axis=1, keepdims=True)
    lane = lax.broadcasted_iota(jnp.int32, (seqs, 128), 1)
    tail = jnp.zeros((seqs, 128), F32)
    for i in range(3):
        digit = square.astype(BF16).astype(F32)
        tail = jnp.where(lane == i, digit, tail)
        square = square - digit
    loaded(0)
    scaled = (attended * mix_gain[...]).astype(BF16)
    branch[t, :, pl.ds(model, 128)] = tail.astype(BF16)
    branch[t, :, pl.ds(0, model)] = mm(scaled, wo[...]).astype(BF16)
    pl.semaphore_wait(barrier, tp + ep - 2)
    exchange = [send(branch.at[t], branch.at[t], br_recv.at[d], tp_peer(d)) for d in reversed(range(1, tp))]

    loaded(1)
    new_keys[...] = mm(normed_in, wk[...]).astype(BF16)
    new_values[...] = mm(normed_in, wv[...]).astype(BF16)
    weights = route_weights[...]
    share = weights / jnp.sum(weights, axis=0, keepdims=True)
    named = route_experts[...]
    diagonal = lax.broadcasted_iota(jnp.int32, (seqs, seqs), 0) == lax.broadcasted_iota(
        jnp.int32, (seqs, seqs), 1
    )
    factors = []
    for x in range(ep):
        line = jnp.sum(jnp.where(named == x, share, 0.0), axis=0, keepdims=True)
        factors.append(jnp.sum(jnp.where(diagonal, line, 0.0), axis=1, keepdims=True))

    for copy in exchange:
        copy.wait_recv()
    head_total = jnp.zeros((seqs, 1), F32)
    summed = jnp.zeros((seqs, model), F32)
    for j in range(tp):
        head_total = head_total + jnp.sum(branch[j, :, pl.ds(model, 128)].astype(F32), axis=1, keepdims=True)
        summed = summed + branch[j, :, pl.ds(0, model)].astype(F32)
    middle = whole + summed * lax.rsqrt(head_total / (tp * span) + eps)
    mid[...] = middle
    normed_mid = (
        middle * lax.rsqrt(jnp.mean(middle * middle, axis=1, keepdims=True) + eps) * ffn_gain[...]
    ).astype(BF16)
    tokens[z, core] = normed_mid

    nearest = [near_first(z, chips, k) for k in range(chips)]
    other = {"ep": 2 * z + 1 - core}
    for k in reversed(range(1, chips)):
        send(tokens.at[z, core], tokens.at[z, core], tok_recv.at[z], {"ep": 2 * nearest[k] + core})
    send(tokens.at[z, core], tokens.at[z, core], fwd_recv.at[z], other)

    for k in range(1, chips):
        s = nearest[k]
        remote(tokens.at[s, core], tokens.at[s, core], tok_recv.at[s], other).wait_recv()
        send(tokens.at[s, core], tokens.at[s, core], fwd_recv.at[s], other)
    loaded(2)
    for k in range(chips):
        s = nearest[k]
        remote(tokens.at[s, 1 - core], tokens.at[s, 1 - core], fwd_recv.at[s], other).wait_recv()
    far = list(reversed(range(chips)))
    inputs = jnp.concatenate([tokens[nearest[k], o].astype(F32) for k in far for o in range(2)], axis=0).astype(BF16)
    gate = jnp.minimum(mm(inputs, gate_w[...]), limit)
    upper = jnp.clip(mm(inputs, up_w[...]), -limit, limit)
    active = ((upper + 1.0) * gate * jax.nn.sigmoid(alpha * gate)).astype(BF16)
    pair = 2 * seqs
    reduce = {}

    def send_piece(i, d):
        part = pl.ds(i * pair, pair)
        reduce[i, d] = send(pieces.at[d, part], arrived.at[d, part], down_recv.at[i, d], tp_peer(d))

    for d in list(reversed(range(1, tp))) + [0]:
        to = peer_of(t, d, tp)
        columns = pl.ds(pl.multiple_of(to * shard, shard), shard)
        pieces[d] = mm(active, down_w[:, columns]).astype(BF16)
        if d:
            send_piece(0, d)
    for i in range(1, chips):
        for d in reversed(range(1, tp)):
            send_piece(i, d)
    for i, k in enumerate(far):
        part = pl.ds(i * pair, pair)
        result = pieces[0, part].astype(F32)
        for d in range(1, tp):
            reduce[i, d].wait_recv()
        for d in range(1, tp):
            result = result + arrived[d, part].astype(F32)
        for o in range(2):
            outs[k, o] = result[o * seqs:(o + 1) * seqs].astype(BF16)
        if k:
            for o in range(2):
                send(outs.at[k, o], back.at[e], ret_recv.at[e], {"ep": 2 * nearest[k] + o})
        else:
            send(outs.at[0, 1 - core], back.at[e], ret_recv.at[e], other)
            back[e] = outs[0, core]

    for i in range(1, ep):
        x = lax.rem(e + i, ep)
        remote(outs.at[0, 0], back.at[x], ret_recv.at[x], other).wait_recv()
    mixture = mid[:, pl.ds(pl.multiple_of(t * shard, shard), shard)]
    for x in range(ep):
        mixture = mixture + factors[x] * back[x].astype(F32)
    mixed[...] = mixture.astype(BF16)
    for copy in sent:
        copy.wait_send()


def hand_out(a, b, c, mixed, new_keys, new_values, sem):
    copies = [
        pltpu.make_async_copy(src, dst, sem.at[i])
        for i, (src, dst) in enumerate(((a, mixed), (b, new_keys), (c, new_values)))
    ]
    for copy in copies:
        copy.start()
    for copy in copies:
        copy.wait()


def body(
    tp, ep,
    resid, attn_gain, w_query, w_key, w_value, key_cache, value_cache, key_bias, lengths,
    mix_gain, w_out, ffn_gain, route_experts, route_weights, w_gate, w_up, w_down,
):
    seqs, heads, width, cache = key_cache.shape
    shard = resid.shape[1]
    model = tp * shard
    span = heads * width
    hidden = w_gate.shape[2]
    top = route_experts.shape[1]
    chips = ep // 2
    vmem = pl.BlockSpec(memory_space=pltpu.VMEM)
    hbm = pl.BlockSpec(memory_space=pl.ANY)
    dma = pltpu.SemaphoreType.DMA
    shapes = ((seqs, shard), (seqs, span), (seqs, span))
    keep = (
        ((tp, seqs, shard), BF16),
        ((1, model), F32),
        ((model, span), BF16),
        ((seqs * span, cache), BF16),
        ((seqs * span, cache), BF16),
        ((seqs * heads, cache), F32),
        ((seqs * heads, 128), jnp.int32),
    )
    first = pl.pallas_call(
        functools.partial(gather, tp),
        out_shape=tuple(pltpu.VMEM(*x) for x in keep),
        in_specs=[hbm] * 7,
        out_specs=(vmem,) * 7,
        scratch_shapes=[
            pltpu.VMEM((seqs, shard), BF16),
            pltpu.SMEM((seqs,), jnp.int32),
            pltpu.VMEM((seqs, heads, cache), F32),
            dma((3,)), dma, dma((tp,)),
        ],
        compiler_params=pltpu.CompilerParams(
            collective_id=0, has_side_effects=True, vmem_limit_bytes=LIMIT_A * 1024 * 1024
        ),
    )(
        resid, lengths, attn_gain.reshape(1, -1), w_query, key_cache.reshape(seqs * span, cache),
        value_cache.reshape(seqs * span, cache), key_bias,
    )
    held = pl.pallas_call(
        functools.partial(layer, tp, ep, heads, width),
        out_shape=tuple(pltpu.VMEM(shape, BF16) for shape in shapes),
        in_specs=[vmem] * 7 + [hbm] * 10,
        out_specs=(vmem, vmem, vmem),
        scratch_shapes=[
            pltpu.VMEM((1, span), F32),
            pltpu.VMEM((1, model), F32),
            pltpu.VMEM((top, seqs), jnp.int32),
            pltpu.VMEM((top, seqs), F32),
            pltpu.VMEM((span, model), BF16),
            pltpu.VMEM((model, hidden), BF16),
            pltpu.VMEM((model, hidden), BF16),
            pltpu.VMEM((model, span), BF16),
            pltpu.VMEM((model, span), BF16),
            pltpu.VMEM((hidden, model), BF16),
            pltpu.VMEM((tp, seqs, model + 128), BF16),
            pltpu.VMEM((seqs, model), F32),
            pltpu.VMEM((chips, 2, seqs, model), BF16),
            pltpu.VMEM((tp, ep * seqs, shard), BF16),
            pltpu.VMEM((tp, ep * seqs, shard), BF16),
            pltpu.VMEM((chips, 2, seqs, shard), BF16),
            pltpu.VMEM((ep, seqs, shard), BF16),
            dma((3,)), dma, dma((tp,)), dma((chips,)), dma((chips,)), dma((chips, tp)), dma((ep,)),
        ],
        compiler_params=pltpu.CompilerParams(
            collective_id=1, has_side_effects=True, vmem_limit_bytes=LIMIT_B * 1024 * 1024
        ),
    )(
        *[pltpu.with_memory_space_constraint(x, pltpu.VMEM) for x in first],
        mix_gain.reshape(1, -1), ffn_gain.reshape(1, -1), route_experts.T, route_weights.T,
        w_out, w_gate, w_up, w_key, w_value, w_down,
    )
    return pl.pallas_call(
        hand_out,
        out_shape=tuple(jax.ShapeDtypeStruct(shape, BF16) for shape in shapes),
        in_specs=[vmem] * 3,
        out_specs=(hbm,) * 3,
        scratch_shapes=[dma((3,))],
    )(*[pltpu.with_memory_space_constraint(x, pltpu.VMEM) for x in held])


def solution(mesh):
    placed = (
        P("ep", "tp"),
        P(),
        P(None, "tp"),
        P(None, "tp"),
        P(None, "tp"),
        P("ep", "tp", None, None),
        P("ep", "tp", None, None),
        P("ep", "tp", None),
        P("ep"),
        P("tp"),
        P("tp", None),
        P(),
        P("ep", None),
        P("ep", None),
        P("ep", None, "tp"),
        P("ep", None, "tp"),
        P("ep", "tp", None),
    )
    return jax.shard_map(
        functools.partial(body, mesh.shape["tp"], mesh.shape["ep"]),
        mesh=mesh,
        in_specs=placed,
        out_specs=(P("ep", "tp"), P("ep", "tp"), P("ep", "tp")),
        check_vma=False,
    )
```
